32 devices in a mesh: ep: 16 (over z, y, x), tp: 2 (over core).
Axes of the slice: x: 2, y: 2, z: 4, core: 2. Of those that a mesh axis runs over, the one named last changes fastest.
Arguments:
- stream: bfloat16 [256, 2048], P('ep', 'tp'), may hold values from -6 to 6
- hidden_state: float32 [256, 2048], P('ep', 'tp'), may hold values from -6 to 6
- conv_state: bfloat16 [256, 3, 2048], P('ep', None, 'tp'), may hold values from -6 to 6
- first_gain: float32 [2048], P('tp'), may hold values from 0.1 to 1.9
- input_weight: bfloat16 [2048, 2048], P('tp', 'ep'), may hold values from -0.125 to 0.125
- branch_weight: bfloat16 [2048, 2048], P('tp', 'ep'), may hold values from -0.125 to 0.125
- conv_taps: bfloat16 [4, 2048], P(None, 'tp'), may hold values from -3 to 3
- recur_gate: bfloat16 [32, 64, 64], P('tp'), may hold values from -0.75 to 0.75
- input_gate: bfloat16 [32, 64, 64], P('tp'), may hold values from -0.75 to 0.75
- decay_logit: float32 [2048], P('tp'), may hold values from 1.5 to 8
- output_weight: bfloat16 [2048, 2048], P('tp', 'ep'), may hold values from -0.25 to 0.25
- second_gain: float32 [2048], P('tp'), may hold values from 0.1 to 1.9
- routes: int32 [256, 2], P('ep'), may hold values from 0 to 3, all different within a row; in each aligned block of 16 rows (0 to 15, 16 to 31, ...) at most 16 rows name the same one
- route_weight: float32 [256, 2], P('ep'), may hold values from 0.25 to 1
- expert_gate: bfloat16 [2048, 12288], P(None, ('ep', 'tp')), may hold values from -0.125 to 0.125
- expert_up: bfloat16 [2048, 12288], P(None, ('ep', 'tp')), may hold values from -0.125 to 0.125
- expert_down: bfloat16 [12288, 2048], P(('ep', 'tp')), may hold values from -0.21875 to 0.21875
Outputs:
- new_stream: bfloat16 [256, 2048], P('ep', 'tp')
- new_hidden: float32 [256, 2048], P('ep', 'tp')
- new_conv: bfloat16 [256, 3, 2048], P('ep', None, 'tp')
The draws below stay inside these ranges and needn't reach their ends.
Inputs may be any that keep to these rules, and one draw needn't show every extreme that they name: `routes`: among the rows of one index of ep, no expert is named more than 16 times; in every draw some expert is named exactly 16 times by the rows of some index. Each row names different experts.
All inputs are finite; a program needn't handle non-finite values.
Results may differ from the reference program's by a relative error of at most 0.022.
Values may be sent and summed in bfloat16 or wider, within the bound.
A program may use at most 128 MiB of HBM per device.

```python
import math
import jax
import jax.numpy as jnp
import numpy as np
from jax import lax

D = 2048
F = 3072
BLOCK = 64
CONV_W = 4
TOPK = 2
SEQ_DEV = 16
SEQS = 256
HEADS = 32
EXPERTS = 4
CAP = 16
N_EP = 16


def levels(key, shape, cuts, smallest, largest):
    gain = 1.0
    for axis_at, shards_of in cuts:
        draws = jax.random.uniform(jax.random.fold_in(jax.random.fold_in(key, 6), axis_at), (shards_of,), jnp.float32, smallest / len(cuts), largest / len(cuts))
        gain = gain * jnp.repeat(jnp.exp(draws), shape[axis_at] // shards_of).reshape((-1,) + (1,) * (len(shape) - 1 - axis_at))
    return gain


def assign_block(key, own, number, rows, amount, top, bound, skew):
    sequence = jax.random.permutation(key, amount)
    packed, common = load_shares(amount, rows * top, bound, skew, True), load_shares(amount, rows * top, bound, skew, False)
    places = jnp.arange(amount)

    def named(lengths, offset_by):
        used = int((lengths > 0).sum())
        fixed = max(1, used // 4)
        shifted = fixed + (places - fixed + offset_by * (used - fixed)) % max(1, amount - fixed)
        return jnp.zeros((amount,), jnp.int32).at[sequence[jnp.where(places < fixed, places, shifted)]].set(jnp.asarray(lengths, jnp.int32))

    lengths = jnp.where(number % 4 == 0, named(packed, number // 4), named(common, number - number // 4 - 1))
    mixed = jax.random.permutation(jax.random.fold_in(own, 3), amount)
    donor, sink = mixed[0:amount // 2 * 2:2], mixed[1:amount // 2 * 2:2]
    margin = jnp.minimum(lengths[donor] - 1, bound - lengths[sink]) // 2
    margin = jnp.where((donor == sequence[0]) | (sink == sequence[0]) | (lengths[sink] == 0), 0, jnp.maximum(margin, 0))
    shifted = jax.random.randint(jax.random.fold_in(own, 4), (amount // 2,), 0, 1 << 20) % (margin + 1)
    lengths = lengths.at[donor].add(-shifted).at[sink].add(shifted)
    members = jnp.searchsorted(jnp.cumsum(lengths), jnp.arange(rows * top), side="right").astype(jnp.int32)
    grid = members.reshape(top, rows).T
    grid = grid[jax.random.permutation(jax.random.fold_in(own, 1), rows)]
    offset_by = jax.random.randint(jax.random.fold_in(own, 2), (rows, 1), 0, top)
    return jnp.take_along_axis(grid, (jnp.arange(top)[None, :] + offset_by) % top, axis=1)


def load_shares(count, total, bound, skew, full):
    loads = [(1 << 20) // math.isqrt(standing ** skew) + 1 for standing in range(1, count + 1)]
    largest = bound if full else min(bound, max(-(-total // count), total * loads[0] // sum(loads)))
    least = 1 if total - largest >= count - 1 else 0
    counts, surplus = [largest] + [least] * (count - 1), total - largest - least * (count - 1)
    while surplus > 0:
        movable = [i for i in range(1, count) if counts[i] < largest] or [i for i in range(1, count) if counts[i] < bound]
        mass, remaining = sum([loads[i] for i in movable]), surplus
        for i in movable:
            more = min(bound - counts[i], max(1, remaining * loads[i] // mass), surplus)
            counts[i] = counts[i] + more
            surplus = surplus - more
    return np.array(counts)


def normal_values(own_key, shape, width, reach, cuts=(), kind=jnp.bfloat16):
    values = width * jax.random.normal(own_key, shape, jnp.float32)
    if cuts:
        values = values * levels(own_key, shape, cuts, -0.22, 0.18)
    return jnp.clip(values, -reach, reach).astype(kind)


def setup_inputs(seed: int = 0) -> dict:
    arg_keys = jax.random.split(jax.random.key(seed), 18)
    stream = normal_values(arg_keys[0], (SEQS, D), 1.0, 6.0, ((0, 16), (1, 2)))
    hidden_state = normal_values(arg_keys[1], (SEQS, D), 1.0, 6.0, ((0, 16), (1, 2)), jnp.float32)
    conv_state = normal_values(arg_keys[2], (SEQS, CONV_W - 1, D), 1.0, 6.0, ((0, 16), (2, 2)))
    first_gain = jnp.clip(1.0 + 0.18 * jax.random.normal(arg_keys[3], (D,), jnp.float32), 0.1, 1.9)
    input_weight = normal_values(arg_keys[4], (D, D), D ** -0.5, 0.125, ((0, 2), (1, 16)))
    branch_weight = normal_values(arg_keys[5], (D, D), D ** -0.5, 0.125, ((0, 2), (1, 16)))
    conv_taps = normal_values(arg_keys[6], (CONV_W, D), 0.5, 3.0, ((1, 2),))
    recur_gate = normal_values(arg_keys[7], (HEADS, BLOCK, BLOCK), BLOCK ** -0.5, 0.75, ((0, 2),))
    input_gate = normal_values(arg_keys[8], (HEADS, BLOCK, BLOCK), BLOCK ** -0.5, 0.75, ((0, 2),))
    decay_logit = jnp.clip(1.5 + 6.5 * jax.random.uniform(arg_keys[9], (D,), jnp.float32) ** levels(arg_keys[9], (D,), ((0, 2),), -0.2, 0.2), 1.5, 8.0)
    output_weight = normal_values(arg_keys[10], (D, D), (D // 4) ** -0.5, 0.25, ((0, 2), (1, 16)))
    second_gain = jnp.clip(1.0 + 0.18 * jax.random.normal(arg_keys[11], (D,), jnp.float32), 0.1, 1.9)
    routes_keys = jax.random.split(jax.random.fold_in(arg_keys[12], 1), SEQS // SEQ_DEV)
    routes_turns = jax.random.permutation(jax.random.fold_in(arg_keys[12], 3), SEQS // SEQ_DEV)
    routes = jax.vmap(lambda own, number: assign_block(jax.random.fold_in(arg_keys[12], 2), own, number, SEQ_DEV, EXPERTS, TOPK, CAP, 1))(routes_keys, routes_turns).reshape((SEQS, TOPK))
    route_weight = jnp.clip(0.25 + 0.75 * jax.random.uniform(arg_keys[13], (SEQS, TOPK), jnp.float32) ** levels(arg_keys[13], (SEQS, TOPK), ((0, 16),), -0.2, 0.2), 0.25, 1.0)
    expert_gate = normal_values(arg_keys[14], (D, EXPERTS * F), D ** -0.5, 0.125, ((1, 32),))
    expert_up = normal_values(arg_keys[15], (D, EXPERTS * F), D ** -0.5, 0.125, ((1, 32),))
    expert_down = normal_values(arg_keys[16], (EXPERTS * F, D), (F // 4) ** -0.5, 0.21875, ((0, 32),))
    return {"stream": stream, "hidden_state": hidden_state, "conv_state": conv_state, "first_gain": first_gain, "input_weight": input_weight, "branch_weight": branch_weight, "conv_taps": conv_taps, "recur_gate": recur_gate, "input_gate": input_gate, "decay_logit": decay_logit, "output_weight": output_weight, "second_gain": second_gain, "routes": routes, "route_weight": route_weight, "expert_gate": expert_gate, "expert_up": expert_up, "expert_down": expert_down}


epsilon = 1e-06
decay_power = 8.0

def block_map(values, table):
    split = values.astype(jnp.float32).reshape(SEQS, HEADS, BLOCK)
    mapped = jnp.einsum('shi,hij->shj', split, table.astype(jnp.float32))
    return mapped.reshape(SEQS, D)

def reference(stream, hidden_state, conv_state, first_gain, input_weight, branch_weight, conv_taps, recur_gate, input_gate, decay_logit, output_weight, second_gain, routes, route_weight, expert_gate, expert_up, expert_down):
    values = stream.astype(jnp.float32)
    first_power = lax.optimization_barrier(jnp.mean(values * values, axis=1, keepdims=True))
    row_scale = lax.rsqrt(first_power + epsilon)
    scaled = (values * first_gain).astype(jnp.bfloat16)
    forward = (jnp.dot(scaled, input_weight, preferred_element_type=jnp.float32) * row_scale).astype(jnp.bfloat16)
    branch = (jnp.dot(scaled, branch_weight, preferred_element_type=jnp.float32) * row_scale).astype(jnp.bfloat16)
    window = jnp.concatenate([conv_state, forward[:, None, :]], axis=1)
    new_conv = window[:, 1:]
    conv_out = jnp.einsum('skc,kc->sc', window.astype(jnp.float32), conv_taps.astype(jnp.float32)).astype(jnp.bfloat16)
    recur_open = jax.nn.sigmoid(block_map(conv_out, recur_gate))
    inward = jax.nn.sigmoid(block_map(conv_out, input_gate))
    log_decay = -decay_power * recur_open * jax.nn.softplus(-decay_logit)
    new_hidden = jnp.exp(log_decay) * hidden_state + jnp.sqrt(-jnp.expm1(2.0 * log_decay)) * (inward * conv_out.astype(jnp.float32))
    mixed = (jax.nn.gelu(branch.astype(jnp.float32)) * new_hidden).astype(jnp.bfloat16)
    middle = (values + jnp.dot(mixed, output_weight, preferred_element_type=jnp.float32)).astype(jnp.bfloat16)
    mid_values = middle.astype(jnp.float32)
    second_power = lax.optimization_barrier(jnp.mean(mid_values * mid_values, axis=1, keepdims=True))
    normed = (mid_values * lax.rsqrt(second_power + epsilon) * second_gain).astype(jnp.bfloat16)
    row_bound = CAP * N_EP

    def one_expert(carry_terms, expert_index):
        chosen = routes == expert_index
        weight = lax.optimization_barrier(jnp.sum(jnp.where(chosen, route_weight, 0.0), axis=1))
        routed = jnp.any(chosen, axis=1)
        rows = jnp.nonzero(routed, size=row_bound, fill_value=0)[0].astype(jnp.int32)
        live_rows = jnp.arange(row_bound) < jnp.sum(routed.astype(jnp.int32))
        picked = normed[rows].astype(jnp.float32)
        start = (expert_index * F).astype(jnp.int32)
        gate_cols = lax.dynamic_slice_in_dim(expert_gate, start, F, 1).astype(jnp.float32)
        up_cols = lax.dynamic_slice_in_dim(expert_up, start, F, 1).astype(jnp.float32)
        down_rows = lax.dynamic_slice_in_dim(expert_down, start, F, 0).astype(jnp.float32)
        gate_act = jnp.dot(picked, gate_cols)
        upper = jnp.dot(picked, up_cols)
        inner = lax.optimization_barrier((jax.nn.silu(gate_act) * upper).astype(jnp.bfloat16)).astype(jnp.float32)
        expert_out = jnp.dot(inner, down_rows)
        factor = jnp.where(live_rows, weight[rows], 0.0)
        return (carry_terms.at[rows].add(expert_out * factor[:, None]), None)
    expert_mix, _ = lax.scan(one_expert, jnp.zeros((SEQS, D), jnp.float32), jnp.arange(EXPERTS, dtype=jnp.int32))
    new_stream = (mid_values + expert_mix).astype(jnp.bfloat16)
    return (new_stream, new_hidden, new_conv)
```

```python
import functools

import jax
import jax.numpy as jnp
from jax import lax
from jax.experimental import pallas as pl
from jax.experimental.pallas import tpu as pltpu
from jax.sharding import PartitionSpec as P

EP_SPAN = 4
PLANE = 4
MESH = pl.DeviceIdType.MESH

epsilon = 1e-06
decay_power = 8.0
bf16 = jnp.bfloat16
f32 = jnp.float32


def kernel(
    n,
    stream,
    hidden,
    conv,
    gain1,
    win_hbm,
    wbr_hbm,
    taps,
    rgate,
    igate,
    decay,
    wout_hbm,
    gain2,
    routes,
    rweight,
    wg_hbm,
    wu_hbm,
    wd_hbm,
    new_stream,
    new_hidden,
    new_conv,
    win,
    wbr,
    wout,
    wg,
    wu,
    wd,
    rdiag,
    idiag,
    wx,
    x1,
    x2,
    x3,
    xp,
    sq,
    pair1s,
    pair1r,
    fin1,
    y1,
    pair2s,
    pair2r,
    fin2,
    y2,
    inner,
    pair3s,
    pair3r,
    keep,
    sums,
    r1,
    t2,
    r2,
    u3,
    r3,
    load_sem,
    wx_s,
    wx_r,
    sq_s,
    sq_r,
    ag_s,
    ag_r,
    pair_s,
    pair_r,
    y_s,
    y_r,
    xp_s,
    xp_r,
    rs_s,
    rs_r,
):
    e = lax.axis_index("ep")
    t = lax.axis_index("tp")
    rows, half = stream.shape
    zn = n // PLANE
    hn = n // 2
    cols = win.shape[1]
    z, low = e // PLANE, e % PLANE
    lx, ly = low % 2, low // 2
    ex = e + 1 - 2 * lx
    ey = e + 2 - 4 * ly
    other = 1 - t
    pending = []

    def rcopy(src, dst, ssem, rsem, ep, tp):
        return pltpu.make_async_remote_copy(
            src_ref=src,
            dst_ref=dst,
            send_sem=ssem,
            recv_sem=rsem,
            device_id=(ep, tp),
            device_id_type=MESH,
        )

    def send(*args):
        c = rcopy(*args)
        c.start()
        pending.append(c)
        return c

    loads = []
    for i, (a, b) in enumerate(
        ((win_hbm, win), (wbr_hbm, wbr), (wout_hbm, wout), (wg_hbm, wg), (wu_hbm, wu), (wd_hbm, wd))
    ):
        c = pltpu.make_async_copy(a, b, load_sem.at[i])
        c.start()
        loads.append(c)

    def gather(buf, p, after=None):
        s, r = ag_s.at[p], ag_r.at[p]
        at = [lax.rem(z - k + zn, zn) for k in range(zn)]
        zc = [None] * zn
        for k in range(1, zn):
            target = lax.rem(e + PLANE * k, n)
            zc[k] = send(buf.at[0, z], buf.at[0, z], s.at[0, k], r.at[0, k], target, t)
        xc, yc, dc = [None] * zn, [None] * zn, [None] * zn

        def diagonal(k):
            if k % 2 == 0:
                xc[k].wait_recv()
                dc[k] = send(buf.at[1, at[k]], buf.at[3, at[k]], s.at[3, k], r.at[3, k], ey, t)
                if after:
                    after(1, at[k], k)
            else:
                yc[k].wait_recv()
                dc[k] = send(buf.at[2, at[k]], buf.at[3, at[k]], s.at[3, k], r.at[3, k], ex, t)
                if after:
                    after(2, at[k], k)

        for k in range(zn):
            if k:
                zc[k].wait_recv()
            xc[k] = send(buf.at[0, at[k]], buf.at[1, at[k]], s.at[1, k], r.at[1, k], ex, t)
            yc[k] = send(buf.at[0, at[k]], buf.at[2, at[k]], s.at[2, k], r.at[2, k], ey, t)
            if after:
                after(0, at[k], k)
            if k:
                diagonal(k - 1)
        diagonal(zn - 1)
        for k in range(zn):
            if k % 2 == 0:
                yc[k].wait_recv()
                if after:
                    after(2, at[k], k)
            else:
                xc[k].wait_recv()
                if after:
                    after(1, at[k], k)
        for k in range(zn):
            dc[k].wait_recv()
            if after:
                after(3, at[k], k)

    values = stream[...].astype(f32)
    x1[0, z] = (values * gain1[...]).astype(bf16)
    sq[0, 0] = jnp.broadcast_to(jnp.sum(values * values, axis=1, keepdims=True), (rows, 128))
    lane = lax.broadcasted_iota(jnp.int32, (rows, 128), 1)
    wrow = jnp.zeros((rows, 128), f32)
    for k in range(routes.shape[1]):
        wrow += jnp.where(lane == routes[:, k : k + 1], rweight[:, k : k + 1], 0.0)
    wx[0, z] = wrow

    def weights_out():
        out = []
        for q in range(PLANE):
            tx = lax.rem(lx + q % 2, 2)
            ty = lax.rem(ly + q // 2, 2)
            for k in range(zn):
                if q == 0 and k == 0:
                    continue
                target = lax.rem(z + k, zn) * PLANE + 2 * ty + tx
                out.append(send(wx.at[0, z], wx.at[q, z], wx_s.at[q, k], wx_r.at[q, k], target, t))
        return out

    sq1 = send(sq.at[0, 0], sq.at[0, 1], sq_s.at[0], sq_r.at[0], e, other)

    def prepare():
        rdiag[...] = jnp.zeros_like(rdiag)
        idiag[...] = jnp.zeros_like(idiag)
        heads, w, _ = rgate.shape
        per = rdiag.shape[1] // w
        for h in range(heads):
            g, o = h // per, (h % per) * w
            rdiag[g, o : o + w, o : o + w] = rgate[h]
            idiag[g, o : o + w, o : o + w] = igate[h]

    gather(x1, 0)
    wxc = weights_out()
    prepare()

    loads[0].wait()
    loads[1].wait()

    def project(x, weights, pairs, pairr, fin, y, p):
        m = len(weights)

        def part(side):
            lhs = x[pl.ds(2 * side, 2)].reshape(hn * rows, half)
            return [jnp.dot(lhs, w[...], preferred_element_type=f32) for w in weights]

        away = part(other)
        for i in range(m):
            pairs[i] = away[i].astype(bf16)
        pc = send(pairs, pairr, pair_s.at[p], pair_r.at[p], e, other)
        mine = part(t)
        pc.wait_recv()
        for i in range(m):
            total = mine[i] + pairr[i].astype(f32)
            fin[:, i] = total.astype(bf16).reshape(hn, rows, cols)
        owner = e // hn
        slot = e - owner * hn
        own = jnp.logical_and(t == 0, owner == 0)
        ycs = []
        for i in range(2):
            for zz in range(zn):
                tx = lax.rem(lx + i, 2)
                ty = lax.rem(ly + t, 2)
                k = lax.rem(z + zz, zn)
                target = k * PLANE + 2 * ty + tx
                b = i * zn + k
                c = rcopy(
                    fin.at[b], y.at[slot], y_s.at[p, i * zn + zz], y_r.at[p, slot], target, owner
                )
                if i == 0 and zz == 0:

                    @pl.when(jnp.logical_not(own))
                    def _():
                        c.start()

                    @pl.when(own)
                    def _():
                        y[slot] = fin[b]
                else:
                    c.start()
                ycs.append(c)
        for j in range(hn):
            c = rcopy(fin.at[0], y.at[j], y_s.at[p, 0], y_r.at[p, j], e, other)

            @pl.when(jnp.logical_not(jnp.logical_and(own, slot == j)))
            def _():
                c.wait_recv()

        def finish():
            for i, c in enumerate(ycs):
                if i == 0:

                    @pl.when(jnp.logical_not(own))
                    def _():
                        c.wait_send()
                else:
                    c.wait_send()

        return [
            jnp.concatenate([y[j, i] for j in range(hn)], axis=1).astype(f32) for i in range(m)
        ], finish

    (fsum, bsum), finish1 = project(x1, (win, wbr), pair1s, pair1r, fin1, y1, 0)
    sq1.wait_recv()
    mean = (sq[0, 0][:, :1] + sq[0, 1][:, :1]) / (2 * half)
    scale = lax.rsqrt(mean + epsilon)
    forward = (fsum * scale).astype(bf16)
    branch = (bsum * scale).astype(bf16).astype(f32)

    width = taps.shape[0]
    acc = forward.astype(f32) * taps[width - 1 : width, :].astype(f32)
    for k in range(width - 1):
        acc += conv[:, k * half : (k + 1) * half].astype(f32) * taps[k : k + 1, :].astype(f32)
    conv_out = acc.astype(bf16)
    if width > 2:
        new_conv[:, : (width - 2) * half] = conv[:, half : (width - 1) * half]
    new_conv[:, (width - 2) * half :] = forward
    groups, gw, _ = rdiag.shape

    def block_map(table):
        return jnp.concatenate(
            [
                jnp.dot(
                    conv_out[:, g * gw : (g + 1) * gw], table[g], preferred_element_type=f32
                )
                for g in range(groups)
            ],
            axis=1,
        )

    recur_open = jax.nn.sigmoid(block_map(rdiag))
    inward = jax.nn.sigmoid(block_map(idiag))
    neg = -decay[...]
    soft = jnp.maximum(neg, 0.0) + jnp.log1p(jnp.exp(-jnp.abs(neg)))
    u = decay_power * recur_open * soft
    th = jnp.tanh(u)
    state = jnp.exp(-u) * hidden[...] + jnp.sqrt(2.0 * th / (1.0 + th)) * (
        inward * conv_out.astype(f32)
    )
    new_hidden[...] = state
    gelu = 0.5 * branch * (1.0 + jnp.tanh(0.7978845608028654 * (branch + 0.044715 * branch * branch * branch)))
    x2[0, z] = (gelu * state).astype(bf16)

    gather(x2, 1)
    loads[2].wait()
    (osum,), finish2 = project(x2, (wout,), pair2s, pair2r, fin2, y2, 1)
    middle = (values + osum).astype(bf16).astype(f32)
    sq[1, 0] = jnp.broadcast_to(jnp.sum(middle * middle, axis=1, keepdims=True), (rows, 128))
    sq2 = send(sq.at[1, 0], sq.at[1, 1], sq_s.at[1], sq_r.at[1], e, other)
    sq2.wait_recv()
    mean = (sq[1, 0][:, :1] + sq[1, 1][:, :1]) / (2 * half)
    x3[0, z] = (middle * lax.rsqrt(mean + epsilon) * gain2[...]).astype(bf16)

    xpc = []

    def relay(q, at, k):
        xpc.append(
            send(x3.at[q, at], xp.at[q, at], xp_s.at[q, k], xp_r.at[q, k], e, other)
        )

    gather(x3, 2, relay)
    loads[3].wait()
    loads[4].wait()
    for c in xpc:
        c.wait_recv()

    mrows = zn * rows
    here, there = pl.ds(pl.multiple_of(t * half, half), half), pl.ds(
        pl.multiple_of(other * half, half), half
    )
    per = EP_SPAN if n >= 2 * EP_SPAN or n == EP_SPAN else n
    expert = e // per
    for c in wxc:
        c.wait_recv()
    loads[5].wait()

    def each(count, body):
        if count == 1:
            body(0)
        else:
            pl.loop(0, count)(body)

    step = min(PLANE, max(1, 256 // mrows))

    def experts(c):
        qs = pl.ds(c * step, step)
        a = x3[qs].reshape(step * mrows, half)
        b = xp[qs].reshape(step * mrows, half)
        gate = jnp.dot(a, wg[here, :], preferred_element_type=f32) + jnp.dot(
            b, wg[there, :], preferred_element_type=f32
        )
        upper = jnp.dot(a, wu[here, :], preferred_element_type=f32) + jnp.dot(
            b, wu[there, :], preferred_element_type=f32
        )
        inner[qs] = (jax.nn.silu(gate) * upper).astype(bf16).reshape(step, mrows, gate.shape[1])

    each(PLANE // step, experts)

    def row_weights(qs):
        full = wx[qs].reshape(step * mrows, 128)
        lanes = lax.broadcasted_iota(jnp.int32, full.shape, 1)
        return jnp.sum(jnp.where(lanes == expert, full, 0.0), axis=1, keepdims=True)

    hw = half // 2

    def store(ref, qs, lanes):
        def run():
            act = inner[qs].reshape(step * mrows, inner.shape[2])
            out = jnp.dot(act, wd[:, lanes], preferred_element_type=f32) * row_weights(qs)
            for i in range(2):
                ref[i, qs] = (
                    out[:, i * hw : (i + 1) * hw].astype(ref.dtype).reshape(step, zn, rows, hw)
                )

        return run

    each(PLANE // step, lambda c: store(pair3s, pl.ds(c * step, step), there)())
    pc = send(pair3s, pair3r, pair_s.at[2], pair_r.at[2], e, other)
    each(PLANE // step, lambda c: store(keep, pl.ds(c * step, step), here)())
    pc.wait_recv()

    def total(i, q):
        return keep[i, q] + pair3r[i, q].astype(f32)

    first = (1, 2)
    rc = [[None, None], [None, None]]
    peers = (ex, ey)
    for i in range(2):
        sums[i, 1] = total(i, 3).astype(bf16)
        rc[i][1] = send(sums.at[i, 1], r1.at[i, 1], rs_s.at[0, i, 1], rs_r.at[0, i, 1], peers[i], t)
    for i in range(2):
        sums[i, 0] = total(i, first[i]).astype(bf16)
        rc[i][0] = send(sums.at[i, 0], r1.at[i, 0], rs_s.at[0, i, 0], rs_r.at[0, i, 0], peers[i], t)
    sc = [None, None]
    for i in range(2):
        rc[i][1].wait_recv()
        t2[i] = (total(i, first[1 - i]) + r1[i, 1].astype(f32)).astype(bf16)
        sc[i] = send(t2.at[i], r2.at[i], rs_s.at[1, i, 0], rs_r.at[1, i, 0], peers[1 - i], t)
    for i in range(2):
        rc[i][0].wait_recv()
        sc[i].wait_recv()
        keep[i, 0] = total(i, 0) + r1[i, 0].astype(f32) + r2[i].astype(f32)
        u3[:, :, i * hw : (i + 1) * hw] = keep[i, 0].astype(bf16)
    zc = []
    for k in range(1, zn):
        dest = lax.rem(z + k, zn)
        zc.append(
            send(u3.at[dest], r3.at[k], rs_s.at[2, 0, k], rs_r.at[2, 0, k], dest * PLANE + low, t)
        )
    mix = jnp.concatenate([keep[0, 0, z], keep[1, 0, z]], axis=1)
    for k in range(1, zn):
        zc[k - 1].wait_recv()
        mix += r3[k].astype(f32)
    new_stream[...] = (middle + mix).astype(bf16)
    finish1()
    finish2()
    for c in pending:
        c.wait_send()


def per_device(
    stream,
    hidden_state,
    conv_state,
    first_gain,
    input_weight,
    branch_weight,
    conv_taps,
    recur_gate,
    input_gate,
    decay_logit,
    output_weight,
    second_gain,
    routes,
    route_weight,
    expert_gate,
    expert_up,
    expert_down,
):
    n = lax.axis_size("ep")
    rows, half = stream.shape
    past = conv_state.shape[1]
    zn, hn = n // PLANE, n // 2
    cols = input_weight.shape[1]
    hidden_units = expert_gate.shape[1]
    heads, block, _ = recur_gate.shape
    gw = max(128, block)
    hw = half // 2
    dma = pltpu.SemaphoreType.DMA
    vm = pltpu.VMEM
    any_spec = pl.BlockSpec(memory_space=pl.ANY)
    vspec = pl.BlockSpec(memory_space=pltpu.VMEM)
    scratch = [
        vm(input_weight.shape, bf16),
        vm(branch_weight.shape, bf16),
        vm(output_weight.shape, bf16),
        vm(expert_gate.shape, bf16),
        vm(expert_up.shape, bf16),
        vm(expert_down.shape, bf16),
        vm((heads * block // gw, gw, gw), bf16),
        vm((heads * block // gw, gw, gw), bf16),
        vm((PLANE, zn, rows, 128), f32),
        vm((PLANE, zn, rows, half), bf16),
        vm((PLANE, zn, rows, half), bf16),
        vm((PLANE, zn, rows, half), bf16),
        vm((PLANE, zn, rows, half), bf16),
        vm((2, 2, rows, 128), f32),
        vm((2, hn * rows, cols), bf16),
        vm((2, hn * rows, cols), bf16),
        vm((hn, 2, rows, cols), bf16),
        vm((hn, 2, rows, cols), bf16),
        vm((1, hn * rows, cols), bf16),
        vm((1, hn * rows, cols), bf16),
        vm((hn, 1, rows, cols), bf16),
        vm((hn, 1, rows, cols), bf16),
        vm((PLANE, zn * rows, hidden_units), bf16),
        vm((2, PLANE, zn, rows, hw), bf16),
        vm((2, PLANE, zn, rows, hw), bf16),
        vm((2, PLANE, zn, rows, hw), f32),
        vm((2, 2, zn, rows, hw), bf16),
        vm((2, 2, zn, rows, hw), bf16),
        vm((2, zn, rows, hw), bf16),
        vm((2, zn, rows, hw), bf16),
        vm((zn, rows, half), bf16),
        vm((zn, rows, half), bf16),
        dma((6,)),
        dma((PLANE, zn)),
        dma((PLANE, zn)),
        dma((2,)),
        dma((2,)),
        dma((3, PLANE, zn)),
        dma((3, PLANE, zn)),
        dma((3,)),
        dma((3,)),
        dma((2, hn)),
        dma((2, hn)),
        dma((PLANE, zn)),
        dma((PLANE, zn)),
        dma((3, 2, max(2, zn))),
        dma((3, 2, max(2, zn))),
    ]
    a, v = any_spec, vspec
    new_stream, new_hidden, new_conv = pl.pallas_call(
        functools.partial(kernel, n),
        name="layer",
        out_shape=(
            jax.ShapeDtypeStruct(stream.shape, bf16),
            jax.ShapeDtypeStruct(stream.shape, f32),
            jax.ShapeDtypeStruct((rows, past * half), bf16),
        ),
        in_specs=[v, v, v, v, a, a, v, v, v, v, a, v, v, v, a, a, a],
        out_specs=(v, v, v),
        scratch_shapes=scratch,
        compiler_params=pltpu.CompilerParams(
            has_side_effects=True, vmem_limit_bytes=60 * 1024 * 1024
        ),
    )(
        stream,
        hidden_state,
        conv_state.reshape(rows, past * half),
        first_gain.reshape(1, half),
        input_weight,
        branch_weight,
        conv_taps,
        recur_gate,
        input_gate,
        decay_logit.reshape(1, half),
        output_weight,
        second_gain.reshape(1, half),
        routes,
        route_weight,
        expert_gate,
        expert_up,
        expert_down,
    )
    return new_stream, new_hidden, new_conv.reshape(rows, past, half)


def solution(mesh):
    placed = (
        P("ep", "tp"),
        P("ep", "tp"),
        P("ep", None, "tp"),
        P("tp"),
        P("tp", "ep"),
        P("tp", "ep"),
        P(None, "tp"),
        P("tp", None, None),
        P("tp", None, None),
        P("tp"),
        P("tp", "ep"),
        P("tp"),
        P("ep", None),
        P("ep", None),
        P(None, ("ep", "tp")),
        P(None, ("ep", "tp")),
        P(("ep", "tp"), None),
    )
    return jax.shard_map(
        per_device,
        mesh=mesh,
        in_specs=placed,
        out_specs=(P("ep", "tp"), P("ep", "tp"), P("ep", None, "tp")),
        check_vma=False,
    )
```

```python
import functools

import jax
import jax.numpy as jnp
from jax import lax
from jax.experimental import pallas as pl
from jax.experimental.pallas import tpu as pltpu
from jax.sharding import PartitionSpec as P

EP_SPAN = 4
PLANE = 4
MESH = pl.DeviceIdType.MESH

epsilon = 1e-06
decay_power = 8.0
bf16 = jnp.bfloat16
f32 = jnp.float32


def kernel(
    n,
    stream,
    hidden,
    conv,
    gain1,
    win_hbm,
    wbr_hbm,
    taps,
    rgate,
    igate,
    decay,
    wout_hbm,
    gain2,
    routes,
    rweight,
    wg_hbm,
    wu_hbm,
    wd_hbm,
    new_stream,
    new_hidden,
    new_conv,
    win,
    wbr,
    wout,
    wg,
    wu,
    wd,
    rdiag,
    idiag,
    wx,
    x1,
    x2,
    x3,
    xp,
    sq,
    pair1s,
    pair1r,
    fin1,
    y1,
    pair2s,
    pair2r,
    fin2,
    y2,
    inner,
    pair3s,
    pair3r,
    keep,
    sums,
    r1,
    t2,
    r2,
    u3,
    r3,
    load_sem,
    wx_s,
    wx_r,
    sq_s,
    sq_r,
    ag_s,
    ag_r,
    pair_s,
    pair_r,
    y_s,
    y_r,
    xp_s,
    xp_r,
    rs_s,
    rs_r,
):
    e = lax.axis_index("ep")
    t = lax.axis_index("tp")
    rows, half = stream.shape
    zn = n // PLANE
    hn = n // 2
    cols = win.shape[1]
    z, low = e // PLANE, e % PLANE
    lx, ly = low % 2, low // 2
    ex = e + 1 - 2 * lx
    ey = e + 2 - 4 * ly
    other = 1 - t
    pending = []

    def rcopy(src, dst, ssem, rsem, ep, tp):
        return pltpu.make_async_remote_copy(
            src_ref=src,
            dst_ref=dst,
            send_sem=ssem,
            recv_sem=rsem,
            device_id=(ep, tp),
            device_id_type=MESH,
        )

    def send(*args):
        c = rcopy(*args)
        c.start()
        pending.append(c)
        return c

    loads = []
    for i, (a, b) in enumerate(
        ((win_hbm, win), (wbr_hbm, wbr), (wout_hbm, wout), (wg_hbm, wg), (wu_hbm, wu), (wd_hbm, wd))
    ):
        c = pltpu.make_async_copy(a, b, load_sem.at[i])
        c.start()
        loads.append(c)

    def gather(buf, p, after=None):
        s, r = ag_s.at[p], ag_r.at[p]
        at = [lax.rem(z - k + zn, zn) for k in range(zn)]
        zc = [None] * zn
        for k in range(1, zn):
            target = lax.rem(e + PLANE * k, n)
            zc[k] = send(buf.at[0, z], buf.at[0, z], s.at[0, k], r.at[0, k], target, t)
        xc, yc, dc = [None] * zn, [None] * zn, [None] * zn

        def diagonal(k):
            if k % 2 == 0:
                xc[k].wait_recv()
                dc[k] = send(buf.at[1, at[k]], buf.at[3, at[k]], s.at[3, k], r.at[3, k], ey, t)
                if after:
                    after(1, at[k], k)
            else:
                yc[k].wait_recv()
                dc[k] = send(buf.at[2, at[k]], buf.at[3, at[k]], s.at[3, k], r.at[3, k], ex, t)
                if after:
                    after(2, at[k], k)

        for k in range(zn):
            if k:
                zc[k].wait_recv()
            xc[k] = send(buf.at[0, at[k]], buf.at[1, at[k]], s.at[1, k], r.at[1, k], ex, t)
            yc[k] = send(buf.at[0, at[k]], buf.at[2, at[k]], s.at[2, k], r.at[2, k], ey, t)
            if after:
                after(0, at[k], k)
            if k:
                diagonal(k - 1)
        diagonal(zn - 1)
        for k in range(zn):
            if k % 2 == 0:
                yc[k].wait_recv()
                if after:
                    after(2, at[k], k)
            else:
                xc[k].wait_recv()
                if after:
                    after(1, at[k], k)
        for k in range(zn):
            dc[k].wait_recv()
            if after:
                after(3, at[k], k)

    values = stream[...].astype(f32)
    x1[0, z] = (values * gain1[...]).astype(bf16)
    sq[0, 0] = jnp.broadcast_to(jnp.sum(values * values, axis=1, keepdims=True), (rows, 128))
    lane = lax.broadcasted_iota(jnp.int32, (rows, 128), 1)
    wrow = jnp.zeros((rows, 128), f32)
    eye = lax.broadcasted_iota(jnp.int32, (rows, rows), 0) == lax.broadcasted_iota(
        jnp.int32, (rows, rows), 1
    )

    def column(row):
        return jnp.sum(jnp.where(eye, row, 0.0), axis=1, keepdims=True)

    for k in range(routes.shape[0]):
        named = column(routes[k : k + 1, :].astype(f32))
        wrow += jnp.where(lane.astype(f32) == named, column(rweight[k : k + 1, :]), 0.0)
    wx[0, z] = wrow

    def weights_out():
        out = []
        for q in range(PLANE):
            tx = lax.rem(lx + q % 2, 2)
            ty = lax.rem(ly + q // 2, 2)
            for k in range(zn):
                if q == 0 and k == 0:
                    continue
                target = lax.rem(z + k, zn) * PLANE + 2 * ty + tx
                out.append(send(wx.at[0, z], wx.at[q, z], wx_s.at[q, k], wx_r.at[q, k], target, t))
        return out

    sq1 = send(sq.at[0, 0], sq.at[0, 1], sq_s.at[0], sq_r.at[0], e, other)

    def prepare():
        rdiag[...] = jnp.zeros_like(rdiag)
        idiag[...] = jnp.zeros_like(idiag)
        heads, w, _ = rgate.shape
        per = rdiag.shape[1] // w
        for h in range(heads):
            g, o = h // per, (h % per) * w
            rdiag[g, o : o + w, o : o + w] = rgate[h]
            idiag[g, o : o + w, o : o + w] = igate[h]

    gather(x1, 0)
    wxc = weights_out()
    prepare()

    loads[0].wait()
    loads[1].wait()

    def project(x, weights, pairs, pairr, fin, y, p):
        m = len(weights)

        def part(side):
            lhs = x[pl.ds(2 * side, 2)].reshape(hn * rows, half)
            return [jnp.dot(lhs, w[...], preferred_element_type=f32) for w in weights]

        away = part(other)
        for i in range(m):
            pairs[i] = away[i].astype(bf16)
        pc = send(pairs, pairr, pair_s.at[p], pair_r.at[p], e, other)
        mine = part(t)
        pc.wait_recv()
        for i in range(m):
            total = mine[i] + pairr[i].astype(f32)
            fin[:, i] = total.astype(bf16).reshape(hn, rows, cols)
        owner = e // hn
        slot = e - owner * hn
        own = jnp.logical_and(t == 0, owner == 0)
        ycs = []
        for i in range(2):
            for zz in range(zn):
                tx = lax.rem(lx + i, 2)
                ty = lax.rem(ly + t, 2)
                k = lax.rem(z + zz, zn)
                target = k * PLANE + 2 * ty + tx
                b = i * zn + k
                c = rcopy(
                    fin.at[b], y.at[slot], y_s.at[p, i * zn + zz], y_r.at[p, slot], target, owner
                )
                if i == 0 and zz == 0:

                    @pl.when(jnp.logical_not(own))
                    def _():
                        c.start()

                    @pl.when(own)
                    def _():
                        y[slot] = fin[b]
                else:
                    c.start()
                ycs.append(c)
        for j in range(hn):
            c = rcopy(fin.at[0], y.at[j], y_s.at[p, 0], y_r.at[p, j], e, other)

            @pl.when(jnp.logical_not(jnp.logical_and(own, slot == j)))
            def _():
                c.wait_recv()

        def finish():
            for i, c in enumerate(ycs):
                if i == 0:

                    @pl.when(jnp.logical_not(own))
                    def _():
                        c.wait_send()
                else:
                    c.wait_send()

        return [
            jnp.concatenate([y[j, i] for j in range(hn)], axis=1).astype(f32) for i in range(m)
        ], finish

    (fsum, bsum), finish1 = project(x1, (win, wbr), pair1s, pair1r, fin1, y1, 0)
    sq1.wait_recv()
    mean = (sq[0, 0][:, :1] + sq[0, 1][:, :1]) / (2 * half)
    scale = lax.rsqrt(mean + epsilon)
    forward = (fsum * scale).astype(bf16)
    branch = (bsum * scale).astype(bf16).astype(f32)

    width = taps.shape[0]
    acc = forward.astype(f32) * taps[width - 1 : width, :].astype(f32)
    for k in range(width - 1):
        acc += conv[k].astype(f32) * taps[k : k + 1, :].astype(f32)
    conv_out = acc.astype(bf16)
    for k in range(width - 2):
        new_conv[k] = conv[k + 1]
    new_conv[width - 2] = forward
    groups, gw, _ = rdiag.shape

    def block_map(table):
        return jnp.concatenate(
            [
                jnp.dot(
                    conv_out[:, g * gw : (g + 1) * gw], table[g], preferred_element_type=f32
                )
                for g in range(groups)
            ],
            axis=1,
        )

    recur_open = jax.nn.sigmoid(block_map(rdiag))
    inward = jax.nn.sigmoid(block_map(idiag))
    neg = -decay[...]
    soft = jnp.maximum(neg, 0.0) + jnp.log1p(jnp.exp(-jnp.abs(neg)))
    u = decay_power * recur_open * soft
    th = jnp.tanh(u)
    state = jnp.exp(-u) * hidden[...] + jnp.sqrt(2.0 * th / (1.0 + th)) * (
        inward * conv_out.astype(f32)
    )
    new_hidden[...] = state
    gelu = 0.5 * branch * (1.0 + jnp.tanh(0.7978845608028654 * (branch + 0.044715 * branch * branch * branch)))
    x2[0, z] = (gelu * state).astype(bf16)

    gather(x2, 1)
    loads[2].wait()
    (osum,), finish2 = project(x2, (wout,), pair2s, pair2r, fin2, y2, 1)
    middle = (values + osum).astype(bf16).astype(f32)
    sq[1, 0] = jnp.broadcast_to(jnp.sum(middle * middle, axis=1, keepdims=True), (rows, 128))
    sq2 = send(sq.at[1, 0], sq.at[1, 1], sq_s.at[1], sq_r.at[1], e, other)
    sq2.wait_recv()
    mean = (sq[1, 0][:, :1] + sq[1, 1][:, :1]) / (2 * half)
    x3[0, z] = (middle * lax.rsqrt(mean + epsilon) * gain2[...]).astype(bf16)

    xpc = []

    def relay(q, at, k):
        xpc.append(
            send(x3.at[q, at], xp.at[q, at], xp_s.at[q, k], xp_r.at[q, k], e, other)
        )

    gather(x3, 2, relay)
    loads[3].wait()
    loads[4].wait()
    for c in xpc:
        c.wait_recv()

    mrows = zn * rows
    here, there = pl.ds(pl.multiple_of(t * half, half), half), pl.ds(
        pl.multiple_of(other * half, half), half
    )
    per = EP_SPAN if n >= 2 * EP_SPAN or n == EP_SPAN else n
    expert = e // per
    for c in wxc:
        c.wait_recv()
    loads[5].wait()

    def each(count, body):
        if count == 1:
            body(0)
        else:
            pl.loop(0, count)(body)

    step = min(PLANE, max(1, 256 // mrows))

    def experts(c):
        qs = pl.ds(c * step, step)
        a = x3[qs].reshape(step * mrows, half)
        b = xp[qs].reshape(step * mrows, half)
        gate = jnp.dot(a, wg[here, :], preferred_element_type=f32) + jnp.dot(
            b, wg[there, :], preferred_element_type=f32
        )
        upper = jnp.dot(a, wu[here, :], preferred_element_type=f32) + jnp.dot(
            b, wu[there, :], preferred_element_type=f32
        )
        inner[qs] = (jax.nn.silu(gate) * upper).astype(bf16).reshape(step, mrows, gate.shape[1])

    each(PLANE // step, experts)

    def row_weights(qs):
        full = wx[qs].reshape(step * mrows, 128)
        lanes = lax.broadcasted_iota(jnp.int32, full.shape, 1)
        return jnp.sum(jnp.where(lanes == expert, full, 0.0), axis=1, keepdims=True)

    hw = half // 2

    def store(ref, qs, lanes):
        def run():
            act = inner[qs].reshape(step * mrows, inner.shape[2])
            out = jnp.dot(act, wd[:, lanes], preferred_element_type=f32) * row_weights(qs)
            for i in range(2):
                ref[i, qs] = (
                    out[:, i * hw : (i + 1) * hw].astype(ref.dtype).reshape(step, zn, rows, hw)
                )

        return run

    each(PLANE // step, lambda c: store(pair3s, pl.ds(c * step, step), there)())
    pc = send(pair3s, pair3r, pair_s.at[2], pair_r.at[2], e, other)
    each(PLANE // step, lambda c: store(keep, pl.ds(c * step, step), here)())
    pc.wait_recv()

    def total(i, q):
        return keep[i, q] + pair3r[i, q].astype(f32)

    first = (1, 2)
    rc = [[None, None], [None, None]]
    peers = (ex, ey)
    for i in range(2):
        sums[i, 1] = total(i, 3).astype(bf16)
        rc[i][1] = send(sums.at[i, 1], r1.at[i, 1], rs_s.at[0, i, 1], rs_r.at[0, i, 1], peers[i], t)
    for i in range(2):
        sums[i, 0] = total(i, first[i]).astype(bf16)
        rc[i][0] = send(sums.at[i, 0], r1.at[i, 0], rs_s.at[0, i, 0], rs_r.at[0, i, 0], peers[i], t)
    sc = [None, None]
    for i in range(2):
        rc[i][1].wait_recv()
        t2[i] = (total(i, first[1 - i]) + r1[i, 1].astype(f32)).astype(bf16)
        sc[i] = send(t2.at[i], r2.at[i], rs_s.at[1, i, 0], rs_r.at[1, i, 0], peers[1 - i], t)
    for i in range(2):
        rc[i][0].wait_recv()
        sc[i].wait_recv()
        keep[i, 0] = total(i, 0) + r1[i, 0].astype(f32) + r2[i].astype(f32)
        u3[:, :, i * hw : (i + 1) * hw] = keep[i, 0].astype(bf16)
    zc = []
    for k in range(1, zn):
        dest = lax.rem(z + k, zn)
        zc.append(
            send(u3.at[dest], r3.at[k], rs_s.at[2, 0, k], rs_r.at[2, 0, k], dest * PLANE + low, t)
        )
    mix = jnp.concatenate([keep[0, 0, z], keep[1, 0, z]], axis=1)
    for k in range(1, zn):
        zc[k - 1].wait_recv()
        mix += r3[k].astype(f32)
    new_stream[...] = (middle + mix).astype(bf16)
    finish1()
    finish2()
    for c in pending:
        c.wait_send()


def hand_over(a, b, c, x, y, z):
    x[...] = a[...]
    y[...] = b[...]
    z[...] = c[...]


def per_device(
    stream,
    hidden_state,
    conv_state,
    first_gain,
    input_weight,
    branch_weight,
    conv_taps,
    recur_gate,
    input_gate,
    decay_logit,
    output_weight,
    second_gain,
    routes,
    route_weight,
    expert_gate,
    expert_up,
    expert_down,
):
    n = lax.axis_size("ep")
    rows, half = stream.shape
    past = conv_state.shape[1]
    zn, hn = n // PLANE, n // 2
    cols = input_weight.shape[1]
    hidden_units = expert_gate.shape[1]
    heads, block, _ = recur_gate.shape
    gw = max(128, block)
    hw = half // 2
    dma = pltpu.SemaphoreType.DMA
    vm = pltpu.VMEM
    any_spec = pl.BlockSpec(memory_space=pl.ANY)
    vspec = pl.BlockSpec(memory_space=pltpu.VMEM)
    scratch = [
        vm(input_weight.shape, bf16),
        vm(branch_weight.shape, bf16),
        vm(output_weight.shape, bf16),
        vm(expert_gate.shape, bf16),
        vm(expert_up.shape, bf16),
        vm(expert_down.shape, bf16),
        vm((heads * block // gw, gw, gw), bf16),
        vm((heads * block // gw, gw, gw), bf16),
        vm((PLANE, zn, rows, 128), f32),
        vm((PLANE, zn, rows, half), bf16),
        vm((PLANE, zn, rows, half), bf16),
        vm((PLANE, zn, rows, half), bf16),
        vm((PLANE, zn, rows, half), bf16),
        vm((2, 2, rows, 128), f32),
        vm((2, hn * rows, cols), bf16),
        vm((2, hn * rows, cols), bf16),
        vm((hn, 2, rows, cols), bf16),
        vm((hn, 2, rows, cols), bf16),
        vm((1, hn * rows, cols), bf16),
        vm((1, hn * rows, cols), bf16),
        vm((hn, 1, rows, cols), bf16),
        vm((hn, 1, rows, cols), bf16),
        vm((PLANE, zn * rows, hidden_units), bf16),
        vm((2, PLANE, zn, rows, hw), bf16),
        vm((2, PLANE, zn, rows, hw), bf16),
        vm((2, PLANE, zn, rows, hw), f32),
        vm((2, 2, zn, rows, hw), bf16),
        vm((2, 2, zn, rows, hw), bf16),
        vm((2, zn, rows, hw), bf16),
        vm((2, zn, rows, hw), bf16),
        vm((zn, rows, half), bf16),
        vm((zn, rows, half), bf16),
        dma((6,)),
        dma((PLANE, zn)),
        dma((PLANE, zn)),
        dma((2,)),
        dma((2,)),
        dma((3, PLANE, zn)),
        dma((3, PLANE, zn)),
        dma((3,)),
        dma((3,)),
        dma((2, hn)),
        dma((2, hn)),
        dma((PLANE, zn)),
        dma((PLANE, zn)),
        dma((3, 2, max(2, zn))),
        dma((3, 2, max(2, zn))),
    ]
    a, v = any_spec, vspec
    new_stream, new_hidden, new_conv = pl.pallas_call(
        functools.partial(kernel, n),
        name="layer",
        out_shape=(
            jax.ShapeDtypeStruct(stream.shape, bf16),
            jax.ShapeDtypeStruct(stream.shape, f32),
            jax.ShapeDtypeStruct((past, rows, half), bf16),
        ),
        in_specs=[v, v, v, v, a, a, v, v, v, v, a, v, v, v, a, a, a],
        out_specs=(v, v, v),
        scratch_shapes=scratch,
        compiler_params=pltpu.CompilerParams(
            has_side_effects=True, vmem_limit_bytes=60 * 1024 * 1024
        ),
    )(
        stream,
        hidden_state,
        conv_state.transpose(1, 0, 2),
        first_gain.reshape(1, half),
        input_weight,
        branch_weight,
        conv_taps,
        recur_gate,
        input_gate,
        decay_logit.reshape(1, half),
        output_weight,
        second_gain.reshape(1, half),
        routes.T,
        route_weight.T,
        expert_gate,
        expert_up,
        expert_down,
    )
    new_stream, new_hidden, new_conv = pl.pallas_call(
        hand_over,
        name="hand_over",
        out_shape=tuple(jax.ShapeDtypeStruct(x.shape, x.dtype) for x in (new_stream, new_hidden, new_conv)),
        in_specs=[v] * 3,
        out_specs=(v,) * 3,
    )(new_stream, new_hidden, new_conv)
    return new_stream, new_hidden, new_conv.transpose(1, 0, 2)


def solution(mesh):
    placed = (
        P("ep", "tp"),
        P("ep", "tp"),
        P("ep", None, "tp"),
        P("tp"),
        P("tp", "ep"),
        P("tp", "ep"),
        P(None, "tp"),
        P("tp", None, None),
        P("tp", None, None),
        P("tp"),
        P("tp", "ep"),
        P("tp"),
        P("ep", None),
        P("ep", None),
        P(None, ("ep", "tp")),
        P(None, ("ep", "tp")),
        P(("ep", "tp"), None),
    )
    return jax.shard_map(
        per_device,
        mesh=mesh,
        in_specs=placed,
        out_specs=(P("ep", "tp"), P("ep", "tp"), P("ep", None, "tp")),
        check_vma=False,
    )
```

```python
import functools

import jax
import jax.numpy as jnp
from jax import lax
from jax.experimental import pallas as pl
from jax.experimental.pallas import tpu as pltpu
from jax.sharding import PartitionSpec as P

EP_SPAN = 4
PLANE = 4
MESH = pl.DeviceIdType.MESH

epsilon = 1e-06
decay_power = 8.0
bf16 = jnp.bfloat16
f32 = jnp.float32


def kernel(
    n,
    stream_hbm,
    hidden_hbm,
    conv_hbm,
    gain1_hbm,
    win_hbm,
    wbr_hbm,
    taps_hbm,
    rgate_hbm,
    igate_hbm,
    decay_hbm,
    wout_hbm,
    gain2_hbm,
    routes_hbm,
    rweight_hbm,
    wg_hbm,
    wu_hbm,
    wd_hbm,
    new_stream_hbm,
    new_hidden_hbm,
    new_conv_hbm,
    stream,
    hidden,
    conv,
    gain1,
    taps,
    rgate,
    igate,
    decay,
    gain2,
    routes,
    rweight,
    new_stream,
    new_hidden,
    new_conv,
    out_sem,
    win,
    wbr,
    wout,
    wg,
    wu,
    wd,
    rdiag,
    idiag,
    wx,
    x1,
    x2,
    x3,
    xp,
    sq,
    pair1s,
    pair1r,
    fin1,
    y1,
    pair2s,
    pair2r,
    fin2,
    y2,
    inner,
    pair3s,
    pair3r,
    keep,
    sums,
    r1,
    t2,
    r2,
    u3,
    r3,
    load_sem,
    wx_s,
    wx_r,
    sq_s,
    sq_r,
    ag_s,
    ag_r,
    pair_s,
    pair_r,
    y_s,
    y_r,
    xp_s,
    xp_r,
    rs_s,
    rs_r,
):
    e = lax.axis_index("ep")
    t = lax.axis_index("tp")
    rows, half = stream.shape
    zn = n // PLANE
    hn = n // 2
    cols = win.shape[1]
    z, low = e // PLANE, e % PLANE
    lx, ly = low % 2, low // 2
    ex = e + 1 - 2 * lx
    ey = e + 2 - 4 * ly
    other = 1 - t
    pending = []

    def rcopy(src, dst, ssem, rsem, ep, tp):
        return pltpu.make_async_remote_copy(
            src_ref=src,
            dst_ref=dst,
            send_sem=ssem,
            recv_sem=rsem,
            device_id=(ep, tp),
            device_id_type=MESH,
        )

    def send(*args):
        c = rcopy(*args)
        c.start()
        pending.append(c)
        return c

    barrier = pltpu.get_barrier_semaphore()
    pl.semaphore_signal(barrier, inc=1, device_id=(e, other), device_id_type=MESH)

    @pl.loop(1, n)
    def _(d):
        peer = lax.rem(e + d, n)
        pl.semaphore_signal(barrier, inc=1, device_id=(peer, t), device_id_type=MESH)
        pl.semaphore_signal(barrier, inc=1, device_id=(peer, other), device_id_type=MESH)

    def load(i, a, b):
        c = pltpu.make_async_copy(a, b, load_sem.at[i])
        c.start()
        return c

    firsts = [
        load(6 + i, a, b)
        for i, (a, b) in enumerate(
            ((stream_hbm, stream), (gain1_hbm, gain1), (routes_hbm, routes), (rweight_hbm, rweight))
        )
    ]
    loads = [load(i, a, b) for i, (a, b) in enumerate(((win_hbm, win), (wbr_hbm, wbr)))]
    smalls = [
        load(10 + i, a, b)
        for i, (a, b) in enumerate(
            (
                (rgate_hbm, rgate),
                (igate_hbm, igate),
                (hidden_hbm, hidden),
                (conv_hbm, conv),
                (taps_hbm, taps),
                (decay_hbm, decay),
                (gain2_hbm, gain2),
            )
        )
    ]
    loads += [
        load(2 + i, a, b)
        for i, (a, b) in enumerate(((wout_hbm, wout), (wg_hbm, wg), (wu_hbm, wu), (wd_hbm, wd)))
    ]
    for c in firsts:
        c.wait()

    near = [sorted(range(zn), key=lambda o: (abs(o - i), o)) for i in range(zn)]
    at = [z]
    for j in range(1, zn):
        pick = near[0][j]
        for i in range(1, zn):
            pick = jnp.where(z == i, near[i][j], pick)
        at.append(pick)
    ed = ex + ey - e
    held = max(2, zn // 2)

    def gather(buf, p, after=None):
        s, r = ag_s.at[p], ag_r.at[p]
        zc, xc, yc, dc = [], [], [], []

        def line(j, peer):
            return rcopy(
                buf.at[0, z], buf.at[0, z], s.at[0, peer], r.at[0, z], peer * PLANE + low, t
            )

        for j in range(1, zn):
            c = line(j, at[j])
            c.start()
            zc.append(c)
        pending.extend(zc)

        def pass_on(j):
            a = at[j]
            xc.append(send(buf.at[0, a], buf.at[1, a], s.at[1, a], r.at[1, a], ex, t))
            yc.append(send(buf.at[0, a], buf.at[2, a], s.at[2, a], r.at[2, a], ey, t))
            if j >= held:
                dc.append(send(buf.at[0, a], buf.at[3, a], s.at[3, a], r.at[3, a], ed, t))

        def relayed(j):
            a = at[j]
            if j % 2 == 0:
                xc[j].wait_recv()
                dc.append(send(buf.at[1, a], buf.at[3, a], s.at[3, a], r.at[3, a], ey, t))
            else:
                yc[j].wait_recv()
                dc.append(send(buf.at[2, a], buf.at[3, a], s.at[3, a], r.at[3, a], ex, t))
            if after:
                after(1 + j % 2, a)

        for j in range(zn):
            a = at[j]
            if j:
                rcopy(buf.at[0, a], buf.at[0, a], s.at[0, a], r.at[0, a], e, other).wait_recv()
            pass_on(j)
            if after:
                after(0, a)
            if 1 <= j <= held:
                relayed(j - 1)
        for j in range(zn):
            a = at[j]
            if j >= held:
                xc[j].wait_recv()
                if after:
                    after(1, a)
                yc[j].wait_recv()
                if after:
                    after(2, a)
            elif j % 2 == 0:
                yc[j].wait_recv()
                if after:
                    after(2, a)
            else:
                xc[j].wait_recv()
                if after:
                    after(1, a)
        for j in range(zn):
            a = at[j]
            rcopy(buf.at[0, a], buf.at[3, a], s.at[3, a], r.at[3, a], e, other).wait_recv()
            if after:
                after(3, a)

    values = stream[...].astype(f32)
    x1[0, z] = (values * gain1[...]).astype(bf16)
    sq[0, 0] = jnp.broadcast_to(jnp.sum(values * values, axis=1, keepdims=True), (rows, 128))
    lane = lax.broadcasted_iota(jnp.int32, (rows, 128), 1)
    wrow = jnp.zeros((rows, 128), f32)
    eye = lax.broadcasted_iota(jnp.int32, (rows, rows), 0) == lax.broadcasted_iota(
        jnp.int32, (rows, rows), 1
    )

    def column(row):
        return jnp.sum(jnp.where(eye, row, 0.0), axis=1, keepdims=True)

    for k in range(routes.shape[0]):
        named = column(routes[k : k + 1, :].astype(f32))
        wrow += jnp.where(lane.astype(f32) == named, column(rweight[k : k + 1, :]), 0.0)
    wx[0, z] = wrow

    def weights_out():
        out = []
        for q in range(PLANE):
            tx = lax.rem(lx + q % 2, 2)
            ty = lax.rem(ly + q // 2, 2)
            for k in range(zn):
                if q == 0 and k == 0:
                    continue
                target = lax.rem(z + k, zn) * PLANE + 2 * ty + tx
                out.append(send(wx.at[0, z], wx.at[q, z], wx_s.at[q, k], wx_r.at[q, k], target, t))
        return out

    pl.semaphore_wait(barrier, 2 * n - 1)
    sq1 = send(sq.at[0, 0], sq.at[0, 1], sq_s.at[0], sq_r.at[0], e, other)

    def prepare():
        rdiag[...] = jnp.zeros_like(rdiag)
        idiag[...] = jnp.zeros_like(idiag)
        heads, w, _ = rgate.shape
        per = rdiag.shape[1] // w
        for h in range(heads):
            g, o = h // per, (h % per) * w
            rdiag[g, o : o + w, o : o + w] = rgate[h]
            idiag[g, o : o + w, o : o + w] = igate[h]

    gather(x1, 0)
    wxc = weights_out()
    for c in smalls:
        c.wait()
    prepare()

    loads[0].wait()
    loads[1].wait()

    def project(x, weights, pairs, pairr, fin, y, p):
        m = len(weights)

        def part(side):
            lhs = x[pl.ds(2 * side, 2)].reshape(hn * rows, half)
            return [jnp.dot(lhs, w[...], preferred_element_type=f32) for w in weights]

        away = part(other)
        for i in range(m):
            pairs[i] = away[i].astype(bf16)
        pc = send(pairs, pairr, pair_s.at[p], pair_r.at[p], e, other)
        mine = part(t)
        pc.wait_recv()
        for i in range(m):
            total = mine[i] + pairr[i].astype(f32)
            fin[:, i] = total.astype(bf16).reshape(hn, rows, cols)
        owner = e // hn
        slot = e - owner * hn
        own = jnp.logical_and(t == 0, owner == 0)
        ycs = []
        for i in range(2):
            for zz in range(zn):
                tx = lax.rem(lx + i, 2)
                ty = lax.rem(ly + t, 2)
                k = lax.rem(z + zz, zn)
                target = k * PLANE + 2 * ty + tx
                b = i * zn + k
                c = rcopy(
                    fin.at[b], y.at[slot], y_s.at[p, i * zn + zz], y_r.at[p, slot], target, owner
                )
                if i == 0 and zz == 0:

                    @pl.when(jnp.logical_not(own))
                    def _():
                        c.start()

                    @pl.when(own)
                    def _():
                        y[slot] = fin[b]
                else:
                    c.start()
                ycs.append(c)
        for j in range(hn):
            c = rcopy(fin.at[0], y.at[j], y_s.at[p, 0], y_r.at[p, j], e, other)

            @pl.when(jnp.logical_not(jnp.logical_and(own, slot == j)))
            def _():
                c.wait_recv()

        def finish():
            for i, c in enumerate(ycs):
                if i == 0:

                    @pl.when(jnp.logical_not(own))
                    def _():
                        c.wait_send()
                else:
                    c.wait_send()

        return [
            jnp.concatenate([y[j, i] for j in range(hn)], axis=1).astype(f32) for i in range(m)
        ], finish

    (fsum, bsum), finish1 = project(x1, (win, wbr), pair1s, pair1r, fin1, y1, 0)
    sq1.wait_recv()
    mean = (sq[0, 0][:, :1] + sq[0, 1][:, :1]) / (2 * half)
    scale = lax.rsqrt(mean + epsilon)
    forward = (fsum * scale).astype(bf16)
    branch = (bsum * scale).astype(bf16).astype(f32)

    width = taps.shape[0]
    acc = forward.astype(f32) * taps[width - 1 : width, :].astype(f32)
    for k in range(width - 1):
        acc += conv[k].astype(f32) * taps[k : k + 1, :].astype(f32)
    conv_out = acc.astype(bf16)
    for k in range(width - 2):
        new_conv[k] = conv[k + 1]
    new_conv[width - 2] = forward
    groups, gw, _ = rdiag.shape

    def block_map(table):
        return jnp.concatenate(
            [
                jnp.dot(
                    conv_out[:, g * gw : (g + 1) * gw], table[g], preferred_element_type=f32
                )
                for g in range(groups)
            ],
            axis=1,
        )

    recur_open = jax.nn.sigmoid(block_map(rdiag))
    inward = jax.nn.sigmoid(block_map(idiag))
    neg = -decay[...]
    soft = jnp.maximum(neg, 0.0) + jnp.log1p(jnp.exp(-jnp.abs(neg)))
    u = decay_power * recur_open * soft
    th = jnp.tanh(u)
    state = jnp.exp(-u) * hidden[...] + jnp.sqrt(2.0 * th / (1.0 + th)) * (
        inward * conv_out.astype(f32)
    )
    new_hidden[...] = state
    outs = [
        pltpu.make_async_copy(a, b, out_sem.at[i])
        for i, (a, b) in enumerate(((new_hidden, new_hidden_hbm), (new_conv, new_conv_hbm)))
    ]
    gelu = 0.5 * branch * (1.0 + jnp.tanh(0.7978845608028654 * (branch + 0.044715 * branch * branch * branch)))
    x2[0, z] = (gelu * state).astype(bf16)

    for c in outs:
        c.start()
    gather(x2, 1)
    loads[2].wait()
    (osum,), finish2 = project(x2, (wout,), pair2s, pair2r, fin2, y2, 1)
    middle = (values + osum).astype(bf16).astype(f32)
    sq[1, 0] = jnp.broadcast_to(jnp.sum(middle * middle, axis=1, keepdims=True), (rows, 128))
    sq2 = send(sq.at[1, 0], sq.at[1, 1], sq_s.at[1], sq_r.at[1], e, other)
    sq2.wait_recv()
    mean = (sq[1, 0][:, :1] + sq[1, 1][:, :1]) / (2 * half)
    x3[0, z] = (middle * lax.rsqrt(mean + epsilon) * gain2[...]).astype(bf16)

    xpc = []

    def relay(q, a):
        xpc.append(send(x3.at[q, a], xp.at[q, a], xp_s.at[q, a], xp_r.at[q, a], e, other))

    gather(x3, 2, relay)
    loads[3].wait()
    loads[4].wait()
    for c in xpc:
        c.wait_recv()

    mrows = zn * rows
    here, there = pl.ds(pl.multiple_of(t * half, half), half), pl.ds(
        pl.multiple_of(other * half, half), half
    )
    per = EP_SPAN if n >= 2 * EP_SPAN or n == EP_SPAN else n
    expert = e // per
    for c in wxc:
        c.wait_recv()
    loads[5].wait()

    def each(count, body):
        if count == 1:
            body(0)
        else:
            pl.loop(0, count)(body)

    step = min(PLANE, max(1, 256 // mrows))

    def experts(c):
        qs = pl.ds(c * step, step)
        a = x3[qs].reshape(step * mrows, half)
        b = xp[qs].reshape(step * mrows, half)
        gate = jnp.dot(a, wg[here, :], preferred_element_type=f32) + jnp.dot(
            b, wg[there, :], preferred_element_type=f32
        )
        upper = jnp.dot(a, wu[here, :], preferred_element_type=f32) + jnp.dot(
            b, wu[there, :], preferred_element_type=f32
        )
        inner[qs] = (jax.nn.silu(gate) * upper).astype(bf16).reshape(step, mrows, gate.shape[1])

    each(PLANE // step, experts)

    hw = half // 2

    def weights_of(q):
        full = wx[q].reshape(mrows, 128)
        lanes = lax.broadcasted_iota(jnp.int32, full.shape, 1)
        return jnp.sum(jnp.where(lanes == expert, full, 0.0), axis=1, keepdims=True)

    def down(ref, q, lanes):
        out = jnp.dot(inner[q], wd[:, lanes], preferred_element_type=f32) * weights_of(q)
        for i in range(2):
            ref[q, i] = out[:, i * hw : (i + 1) * hw].astype(ref.dtype).reshape(zn, rows, hw)

    pcs = {}
    for q in (3, 1, 2, 0):
        down(pair3s, q, there)
        pcs[q] = send(pair3s.at[q], pair3r.at[q], pair_s.at[2 + q], pair_r.at[2 + q], e, other)
    for q in (3, 1, 2, 0):
        down(keep, q, here)

    def total(i, q):
        return keep[q, i] + pair3r[q, i].astype(f32)

    first = (1, 2)
    rc = [[None, None], [None, None]]
    peers = (ex, ey)
    pcs[3].wait_recv()
    for i in range(2):
        sums[i, 1] = total(i, 3).astype(bf16)
        rc[i][1] = send(sums.at[i, 1], r1.at[i, 1], rs_s.at[0, i, 1], rs_r.at[0, i, 1], peers[i], t)
    pcs[1].wait_recv()
    pcs[2].wait_recv()
    for i in range(2):
        sums[i, 0] = total(i, first[i]).astype(bf16)
        rc[i][0] = send(sums.at[i, 0], r1.at[i, 0], rs_s.at[0, i, 0], rs_r.at[0, i, 0], peers[i], t)
    pcs[0].wait_recv()
    sc = [None, None]
    for i in range(2):
        rc[i][1].wait_recv()
        t2[i] = (total(i, first[1 - i]) + r1[i, 1].astype(f32)).astype(bf16)
        sc[i] = send(t2.at[i], r2.at[i], rs_s.at[1, i, 0], rs_r.at[1, i, 0], peers[1 - i], t)
    for i in range(2):
        rc[i][0].wait_recv()
        sc[i].wait_recv()
        keep[0, i] = total(i, 0) + r1[i, 0].astype(f32) + r2[i].astype(f32)
        u3[:, :, i * hw : (i + 1) * hw] = keep[0, i].astype(bf16)
    zc = []
    for k in range(1, zn):
        dest = lax.rem(z + k, zn)
        zc.append(
            send(u3.at[dest], r3.at[k], rs_s.at[2, 0, k], rs_r.at[2, 0, k], dest * PLANE + low, t)
        )
    mix = jnp.concatenate([keep[0, 0, z], keep[0, 1, z]], axis=1)
    for k in range(1, zn):
        zc[k - 1].wait_recv()
        mix += r3[k].astype(f32)
    new_stream[...] = (middle + mix).astype(bf16)
    outs.append(pltpu.make_async_copy(new_stream, new_stream_hbm, out_sem.at[2]))
    outs[2].start()
    finish1()
    finish2()
    for c in pending:
        c.wait_send()
    for c in outs:
        c.wait()


def hand_over(a, b, c, x, y, z):
    x[...] = a[...]
    y[...] = b[...]
    z[...] = c[...]


def per_device(
    stream,
    hidden_state,
    conv_state,
    first_gain,
    input_weight,
    branch_weight,
    conv_taps,
    recur_gate,
    input_gate,
    decay_logit,
    output_weight,
    second_gain,
    routes,
    route_weight,
    expert_gate,
    expert_up,
    expert_down,
):
    n = lax.axis_size("ep")
    rows, half = stream.shape
    past = conv_state.shape[1]
    zn, hn = n // PLANE, n // 2
    cols = input_weight.shape[1]
    hidden_units = expert_gate.shape[1]
    heads, block, _ = recur_gate.shape
    gw = max(128, block)
    hw = half // 2
    dma = pltpu.SemaphoreType.DMA
    vm = pltpu.VMEM
    any_spec = pl.BlockSpec(memory_space=pl.ANY)
    vspec = pl.BlockSpec(memory_space=pltpu.VMEM)
    top = routes.shape[1]
    scratch = [
        vm(stream.shape, bf16),
        vm(stream.shape, f32),
        vm((past, rows, half), bf16),
        vm((1, half), f32),
        vm(conv_taps.shape, bf16),
        vm(recur_gate.shape, bf16),
        vm(input_gate.shape, bf16),
        vm((1, half), f32),
        vm((1, half), f32),
        vm((top, rows), jnp.int32),
        vm((top, rows), f32),
        vm(stream.shape, bf16),
        vm(stream.shape, f32),
        vm((past, rows, half), bf16),
        dma((3,)),
        vm(input_weight.shape, bf16),
        vm(branch_weight.shape, bf16),
        vm(output_weight.shape, bf16),
        vm(expert_gate.shape, bf16),
        vm(expert_up.shape, bf16),
        vm(expert_down.shape, bf16),
        vm((heads * block // gw, gw, gw), bf16),
        vm((heads * block // gw, gw, gw), bf16),
        vm((PLANE, zn, rows, 128), f32),
        vm((PLANE, zn, rows, half), bf16),
        vm((PLANE, zn, rows, half), bf16),
        vm((PLANE, zn, rows, half), bf16),
        vm((PLANE, zn, rows, half), bf16),
        vm((2, 2, rows, 128), f32),
        vm((2, hn * rows, cols), bf16),
        vm((2, hn * rows, cols), bf16),
        vm((hn, 2, rows, cols), bf16),
        vm((hn, 2, rows, cols), bf16),
        vm((1, hn * rows, cols), bf16),
        vm((1, hn * rows, cols), bf16),
        vm((hn, 1, rows, cols), bf16),
        vm((hn, 1, rows, cols), bf16),
        vm((PLANE, zn * rows, hidden_units), bf16),
        vm((PLANE, 2, zn, rows, hw), bf16),
        vm((PLANE, 2, zn, rows, hw), bf16),
        vm((PLANE, 2, zn, rows, hw), f32),
        vm((2, 2, zn, rows, hw), bf16),
        vm((2, 2, zn, rows, hw), bf16),
        vm((2, zn, rows, hw), bf16),
        vm((2, zn, rows, hw), bf16),
        vm((zn, rows, half), bf16),
        vm((zn, rows, half), bf16),
        dma((17,)),
        dma((PLANE, zn)),
        dma((PLANE, zn)),
        dma((2,)),
        dma((2,)),
        dma((3, PLANE, zn)),
        dma((3, PLANE, zn)),
        dma((6,)),
        dma((6,)),
        dma((2, hn)),
        dma((2, hn)),
        dma((PLANE, zn)),
        dma((PLANE, zn)),
        dma((3, 2, max(2, zn))),
        dma((3, 2, max(2, zn))),
    ]
    a, v = any_spec, vspec
    new_stream, new_hidden, new_conv = pl.pallas_call(
        functools.partial(kernel, n),
        name="layer",
        out_shape=(
            jax.ShapeDtypeStruct(stream.shape, bf16),
            jax.ShapeDtypeStruct(stream.shape, f32),
            jax.ShapeDtypeStruct((past, rows, half), bf16),
        ),
        in_specs=[a] * 17,
        out_specs=(a, a, a),
        scratch_shapes=scratch,
        compiler_params=pltpu.CompilerParams(
            collective_id=0, has_side_effects=True, vmem_limit_bytes=60 * 1024 * 1024
        ),
    )(
        stream,
        hidden_state,
        conv_state.transpose(1, 0, 2),
        first_gain.reshape(1, half),
        input_weight,
        branch_weight,
        conv_taps,
        recur_gate,
        input_gate,
        decay_logit.reshape(1, half),
        output_weight,
        second_gain.reshape(1, half),
        routes.T,
        route_weight.T,
        expert_gate,
        expert_up,
        expert_down,
    )
    new_stream, new_hidden, new_conv = pl.pallas_call(
        hand_over,
        name="hand_over",
        out_shape=tuple(jax.ShapeDtypeStruct(x.shape, x.dtype) for x in (new_stream, new_hidden, new_conv)),
        in_specs=[v] * 3,
        out_specs=(v,) * 3,
    )(new_stream, new_hidden, new_conv)
    return new_stream, new_hidden, new_conv.transpose(1, 0, 2)


def solution(mesh):
    placed = (
        P("ep", "tp"),
        P("ep", "tp"),
        P("ep", None, "tp"),
        P("tp"),
        P("tp", "ep"),
        P("tp", "ep"),
        P(None, "tp"),
        P("tp", None, None),
        P("tp", None, None),
        P("tp"),
        P("tp", "ep"),
        P("tp"),
        P("ep", None),
        P("ep", None),
        P(None, ("ep", "tp")),
        P(None, ("ep", "tp")),
        P(("ep", "tp"), None),
    )
    return jax.shard_map(
        per_device,
        mesh=mesh,
        in_specs=placed,
        out_specs=(P("ep", "tp"), P("ep", "tp"), P("ep", None, "tp")),
        check_vma=False,
    )
```
